32 devices in a mesh: sp: 8 (over z, x), tp: 4 (over y, core).
Axes of the slice: x: 2, y: 2, z: 4, core: 2. Of those that a mesh axis runs over, the one named last changes fastest.
Arguments:
- queries: bfloat16 [2048, 2048], P('sp', 'tp'), may hold values from -6 to 6
- keys: bfloat16 [2048, 1024], P('sp', 'tp'), may hold values from -6 to 6
- values: bfloat16 [2048, 1024], P('sp', 'tp'), may hold values from -6 to 6
- docs: int32 [2048], P('sp'), may hold values from 0 to 2, never falling along the last dimension, each value on 1 to 1280 neighbouring positions
- query_gain: float32 [64], replicated, may hold values from 0.5 to 8
- key_gain: float32 [64], replicated, may hold values from 0.5 to 8
- out_weight: bfloat16 [2048, 2048], P('tp'), may hold values from -0.125 to 0.125
- residual: bfloat16 [2048, 2048], P('sp', 'tp'), may hold values from -12 to 12
- norm_gain: float32 [2048], P('tp'), may hold values from 0.1 to 1.9
- routes: int32 [2048, 2], P('sp'), may hold values from 0 to 7, all different within a row; in each aligned block of 256 rows (0 to 255, 256 to 511, ...) at most 80 rows name the same one
- route_weight: float32 [2048, 2], P('sp'), may hold values from 0.1 to 1
- gate_weight: bfloat16 [8, 2048, 4096], P('sp', None, 'tp'), may hold values from -0.3125 to 0.3125
- up_weight: bfloat16 [8, 2048, 4096], P('sp', None, 'tp'), may hold values from -0.3125 to 0.3125
- down_weight: bfloat16 [8, 4096, 2048], P('sp', 'tp'), may hold values from -0.09375 to 0.09375
Outputs:
- mixed: bfloat16 [2048, 2048], P('sp', 'tp')
The draws below stay inside these ranges and needn't reach their ends.
Inputs may be any that keep to these rules, and one draw needn't show every extreme that they name: `routes`: in each aligned block of 256 rows no expert is named by more than 80 rows, and 80 is reached in some block; a row names 2 different experts. `docs`: document numbers never fall along the sequence; a document holds at most 1280 positions.
All inputs are finite; a program needn't handle non-finite values.
Results may differ from the reference program's by a relative error of at most 0.028.
The reference program's roundings to bfloat16 on the way count: a program that leaves them out, or rounds other values in their place, can miss the bound.
Values may be sent and summed in bfloat16 or wider, within the bound.
A program may use at most 64 MiB of HBM per device.

```python
import math
import jax
import jax.numpy as jnp
import numpy as np
from jax import lax

D = 2048
QH = 32
KVH = 16
HD = 64
EFF = 4096
TOPK = 2
GRID_W = 64
DOCS = 3
TOK_DEV = 256
SEQ = 2048
EXPERTS = 8
CAP = 80
DOC_MOST = 1280
N_SP = 8
N_TP = 4


def base_queries(key):
    raw = jax.random.normal(jax.random.fold_in(key, 11), (SEQ, QH * HD), jnp.float32)
    return jnp.clip(raw, -6.0, 6.0)


def draw_queries(key, part):
    return base_queries(key).astype(jnp.bfloat16)


def draw_keys(key, part):
    entries = jnp.clip(jax.random.normal(jax.random.fold_in(key, 12), (SEQ, KVH * HD), jnp.float32), -6.0, 6.0)
    return entries.astype(jnp.bfloat16)


def draw_query_gain(key, part):
    return jax.random.uniform(jax.random.fold_in(key, 21), (HD,), jnp.float32, 0.5, 1.5)


def draw_key_gain(key, part):
    return jax.random.uniform(jax.random.fold_in(key, 22), (HD,), jnp.float32, 0.5, 1.5)


def draw_residual(key, part):
    column = jnp.arange(D, dtype=jnp.float32) / D
    entries = jnp.clip(jax.random.normal(jax.random.fold_in(key, 31), (SEQ, D), jnp.float32), -4.0, 4.0)
    column_scale = jnp.exp(column * math.log(3.0))
    row_scale = jnp.exp(jax.random.uniform(jax.random.fold_in(key, 32), (SEQ, 1), jnp.float32, math.log(0.1), 0.0))
    return (entries * row_scale * column_scale[None, :]).astype(jnp.bfloat16)


def shard_levels(rng, dims, shards, least, largest):
    factor_of, own = 1.0, jax.random.fold_in(rng, 6)
    for dim, shards_of in shards:
        draws = jnp.exp(jax.random.uniform(jax.random.fold_in(own, dim), (shards_of,), jnp.float32, least / len(shards), largest / len(shards)))
        factor_of = factor_of * jnp.repeat(draws, dims[dim] // shards_of).reshape([-1 if axis == dim else 1 for axis in range(len(dims))])
    return factor_of


def split_up(count, total, reach, skew):
    loads = [(1 << 20) // math.isqrt(grade ** skew) + 1 for grade in range(2, count + 1)]
    surplus, given = total - reach - (count - 1), [1] * (count - 1)
    while surplus > 0:
        free = [i for i in range(count - 1) if given[i] < reach]
        mass, remaining = sum([loads[i] for i in free]), surplus
        for i in free:
            more = min(reach - given[i], max(1, remaining * loads[i] // mass), surplus)
            given[i] = given[i] + more
            surplus = surplus - more
    return np.array([reach] + given)


def uneven(own_key, count, total, bound, skew):
    if count == 2:
        one = jax.random.randint(own_key, (), max(1, total - bound), min(bound, total - 1) + 1)
        return jnp.stack([one, total - one])
    sizes = jnp.asarray(split_up(count, total, bound, skew), jnp.int32)
    twos = (count - 1) // 2
    giver, receiver = sizes[1:1 + 2 * twos:2], sizes[2:2 + 2 * twos:2]
    margin = jnp.minimum(giver - 1, bound - receiver)
    moved = jax.random.randint(jax.random.fold_in(own_key, 1), (twos,), 0, 1 << 20) % (margin + 1)
    sizes = sizes.at[1:1 + 2 * twos:2].set(giver - moved).at[2:2 + 2 * twos:2].set(receiver + moved)
    return sizes[jax.random.permutation(jax.random.fold_in(own_key, 2), count)]


def assign_block(stream_key, own, number, rows, count, top, bound, slope):
    ranking = jax.random.permutation(stream_key, count)
    crowded, usual = load_shares(count, rows * top, bound, slope, True), load_shares(count, rows * top, bound, slope, False)
    places = jnp.arange(count)

    def named(lengths, turn):
        used = int((lengths > 0).sum())
        fixed = max(1, used // 4)
        shifted = fixed + (places - fixed + turn * (used - fixed)) % max(1, count - fixed)
        return jnp.zeros((count,), jnp.int32).at[ranking[jnp.where(places < fixed, places, shifted)]].set(jnp.asarray(lengths, jnp.int32))

    lengths = jnp.where(number % 4 == 0, named(crowded, number // 4), named(usual, number - number // 4 - 1))
    mixed = jax.random.permutation(jax.random.fold_in(own, 3), count)
    donor, receiver = mixed[0:count // 2 * 2:2], mixed[1:count // 2 * 2:2]
    room = jnp.minimum(lengths[donor] - 1, bound - lengths[receiver]) // 2
    room = jnp.where((donor == ranking[0]) | (receiver == ranking[0]) | (lengths[receiver] == 0), 0, jnp.maximum(room, 0))
    shifted = jax.random.randint(jax.random.fold_in(own, 4), (count // 2,), 0, 1 << 20) % (room + 1)
    lengths = lengths.at[donor].add(-shifted).at[receiver].add(shifted)
    items = jnp.searchsorted(jnp.cumsum(lengths), jnp.arange(rows * top), side="right").astype(jnp.int32)
    grid = items.reshape(top, rows).T
    grid = grid[jax.random.permutation(jax.random.fold_in(own, 1), rows)]
    turn = jax.random.randint(jax.random.fold_in(own, 2), (rows, 1), 0, top)
    return jnp.take_along_axis(grid, (jnp.arange(top)[None, :] + turn) % top, axis=1)


def load_shares(count, total, most, slope, full):
    weights = [(1 << 20) // math.isqrt(grade ** slope) + 1 for grade in range(1, count + 1)]
    largest = most if full else min(most, max(-(-total // count), total * weights[0] // sum(weights)))
    least = 1 if total - largest >= count - 1 else 0
    counts, surplus = [largest] + [least] * (count - 1), total - largest - least * (count - 1)
    while surplus > 0:
        movable = [i for i in range(1, count) if counts[i] < largest] or [i for i in range(1, count) if counts[i] < most]
        pool, budget = sum([weights[i] for i in movable]), surplus
        for i in movable:
            addition = min(most - counts[i], max(1, budget * weights[i] // pool), surplus)
            counts[i] = counts[i] + addition
            surplus = surplus - addition
    return np.array(counts)


def normal_values(stream_key, dims, spread, most, cuts=(), kind=jnp.bfloat16):
    values = jax.random.normal(stream_key, dims, jnp.float32) * spread
    if len(cuts) > 0:
        values = shard_levels(stream_key, dims, cuts, -0.22, 0.18) * values
    return jnp.clip(values, min=-most, max=most).astype(kind)


def setup_inputs(seed: int = 0) -> dict:
    arg_keys = jax.random.split(jax.random.key(seed), 15)
    queries = draw_queries(jax.random.fold_in(arg_keys[14], 71), 0)
    keys = draw_keys(jax.random.fold_in(arg_keys[14], 71), 0)
    values = normal_values(arg_keys[2], (SEQ, KVH * HD), 1.0, 6.0, ((0, 8), (1, 4)))
    docs = jnp.searchsorted(jnp.cumsum(uneven(arg_keys[3], DOCS, SEQ, DOC_MOST, 0)), jnp.arange(SEQ), side="right").astype(jnp.int32)
    query_gain = draw_query_gain(jax.random.fold_in(arg_keys[14], 71), 0)
    key_gain = draw_key_gain(jax.random.fold_in(arg_keys[14], 71), 0)
    out_weight = normal_values(arg_keys[6], (QH * HD, D), (QH * HD) ** -0.5, 0.125, ((0, 4),))
    residual = draw_residual(jax.random.fold_in(arg_keys[14], 71), 0)
    norm_gain = jnp.clip(1.0 + 0.18 * jax.random.normal(arg_keys[8], (D,), jnp.float32), 0.1, 1.9)
    routes_keys = jax.random.split(jax.random.fold_in(arg_keys[9], 1), SEQ // TOK_DEV)
    routes_turns = jax.random.permutation(jax.random.fold_in(arg_keys[9], 3), SEQ // TOK_DEV)
    routes = jax.vmap(lambda own, number: assign_block(jax.random.fold_in(arg_keys[9], 2), own, number, TOK_DEV, EXPERTS, TOPK, CAP, 2))(routes_keys, routes_turns).reshape((SEQ, TOPK))
    route_weight = jnp.clip(jnp.exp(math.log(1.0) - 2.3025851 * jax.random.uniform(arg_keys[10], (SEQ, TOPK), jnp.float32) ** shard_levels(arg_keys[10], (SEQ, TOPK), ((0, 8),), -0.2, 0.2)), 0.1, 1.0)
    gate_weight = normal_values(arg_keys[11], (EXPERTS, D, EFF), (D // 6) ** -0.5, 0.3125, ((0, 8), (2, 4)))
    up_weight = normal_values(arg_keys[12], (EXPERTS, D, EFF), (D // 6) ** -0.5, 0.3125, ((0, 8), (2, 4)))
    down_weight = normal_values(arg_keys[13], (EXPERTS, EFF, D), EFF ** -0.5, 0.09375, ((0, 8), (1, 4)))
    return {"queries": queries, "keys": keys, "values": values, "docs": docs, "query_gain": query_gain, "key_gain": key_gain, "out_weight": out_weight, "residual": residual, "norm_gain": norm_gain, "routes": routes, "route_weight": route_weight, "gate_weight": gate_weight, "up_weight": up_weight, "down_weight": down_weight}


EPSILON = 1e-06
NEG_BIG = -1e+30
ROTARY_BASE = 10000.0
CLAMP_LIMIT = 7.0
SIGMOID_SCALE = 1.702

def rope_tables(positions, head_dim):
    quarter = head_dim // 4
    freqs = ROTARY_BASE ** (-jnp.arange(quarter, dtype=jnp.float32) / quarter)
    row_pos = (positions // GRID_W).astype(jnp.float32)
    col_pos = (positions % GRID_W).astype(jnp.float32)
    angle = jnp.concatenate([row_pos[:, None] * freqs, col_pos[:, None] * freqs], axis=1)
    return (jnp.cos(angle), jnp.sin(angle))

def norm_rotate(heads, gain, cosine_table, sine_table):
    entries = heads.astype(jnp.float32)
    entries = entries * lax.rsqrt(lax.optimization_barrier(jnp.mean(entries * entries, axis=-1, keepdims=True)) + EPSILON) * gain
    pairs = entries.reshape(entries.shape[:-1] + (entries.shape[-1] // 2, 2))
    first = pairs[..., 0]
    second = pairs[..., 1]
    cos_rows = cosine_table[:, None, :]
    sin_rows = sine_table[:, None, :]
    turned = jnp.stack([first * cos_rows - second * sin_rows, first * sin_rows + second * cos_rows], axis=-1)
    return turned.reshape(heads.shape).astype(jnp.bfloat16)

def clamped_unit(gate_pre, up_pre):
    bounded = jnp.minimum(gate_pre, CLAMP_LIMIT)
    linear = jnp.clip(up_pre, -CLAMP_LIMIT, CLAMP_LIMIT)
    return (bounded * jax.nn.sigmoid(SIGMOID_SCALE * bounded) * (linear + 1.0)).astype(jnp.bfloat16)

def round_trip(term):
    narrow = lax.optimization_barrier(term.astype(jnp.bfloat16))
    return narrow.astype(jnp.float32)

def reference(queries, keys, values, docs, query_gain, key_gain, out_weight, residual, norm_gain, routes, route_weight, gate_weight, up_weight, down_weight):
    positions = jnp.arange(SEQ, dtype=jnp.int32)
    cosine_table, sine_table = rope_tables(positions, HD)
    query_rot = norm_rotate(queries.reshape(SEQ, QH, HD), query_gain, cosine_table, sine_table)
    key_rot = norm_rotate(keys.reshape(SEQ, KVH, HD), key_gain, cosine_table, sine_table)
    query_grouped = jnp.transpose(query_rot.reshape(SEQ, KVH, 2, HD), (1, 0, 2, 3))
    key_grouped = jnp.transpose(key_rot, (1, 0, 2))
    value_grouped = jnp.transpose(values.reshape(SEQ, KVH, HD), (1, 0, 2))
    block_rows = math.gcd(SEQ, 1024)
    score_scale = HD ** (-0.5)

    def one_head(inputs):
        head_queries, head_keys, head_values = inputs
        keys_wide = head_keys.astype(jnp.float32)
        values_wide = head_values.astype(jnp.float32)

        def one_block(index):
            start = (index * block_rows).astype(jnp.int32)
            block_queries = lax.dynamic_slice_in_dim(head_queries, start, block_rows, 0).astype(jnp.float32)
            block_docs = lax.dynamic_slice_in_dim(docs, start, block_rows, 0)
            scores = jnp.einsum('qgd,kd->qgk', block_queries, keys_wide) * score_scale
            allowed = block_docs[:, None, None] == docs[None, None, :]
            scores = jnp.where(allowed, scores, NEG_BIG)
            row_peak = lax.optimization_barrier(jnp.max(scores, axis=-1, keepdims=True))
            weights = jnp.where(allowed, jnp.exp(scores - row_peak), 0.0)
            denominator = lax.optimization_barrier(jnp.sum(weights, axis=-1))
            numerator = jnp.einsum('qgk,kd->qgd', round_trip(weights), values_wide)
            return (numerator / denominator[..., None]).astype(jnp.bfloat16)
        return lax.map(one_block, jnp.arange(SEQ // block_rows, dtype=jnp.int32))
    heads_out = lax.map(one_head, (query_grouped, key_grouped, value_grouped))
    attended = jnp.transpose(heads_out.reshape(KVH, SEQ, 2, HD), (1, 0, 2, 3)).reshape(SEQ, QH * HD)
    group_width = QH * HD // N_TP
    grouped_attn = jnp.transpose(attended.reshape(SEQ, N_TP, group_width), (1, 0, 2))
    grouped_weight = out_weight.reshape(N_TP, group_width, D)

    def add_group(running, inputs):
        part_attn, part_weight = inputs
        return (running + round_trip(jnp.dot(part_attn, part_weight, preferred_element_type=jnp.float32)), None)
    projected, _ = lax.scan(add_group, jnp.zeros((SEQ, D), jnp.float32), (grouped_attn, grouped_weight))
    mixed_first = residual.astype(jnp.float32) + projected
    normed = (mixed_first * lax.rsqrt(lax.optimization_barrier(jnp.mean(mixed_first * mixed_first, axis=1, keepdims=True)) + EPSILON) * norm_gain).astype(jnp.bfloat16)
    pair_count = TOK_DEV * TOPK
    group_routes = routes.reshape(N_SP, pair_count)
    expert_ids = jnp.arange(EXPERTS, dtype=jnp.int32)
    onehot = (group_routes[:, :, None] == expert_ids[None, None, :]).astype(jnp.int32)
    earlier = jnp.cumsum(onehot, axis=1) - onehot
    slot_index = lax.optimization_barrier(jnp.sum(earlier * onehot, axis=2))
    slot_ids = jnp.arange(CAP, dtype=jnp.int32)
    matches = (group_routes[:, :, None, None] == expert_ids[None, None, :, None]) & (slot_index[:, :, None, None] == slot_ids[None, None, None, :])
    entry_ids = jnp.arange(pair_count, dtype=jnp.int32)
    source_entry = lax.optimization_barrier(jnp.sum(jnp.where(matches, entry_ids[None, :, None, None], 0), axis=1))
    occupied = jnp.any(matches, axis=1)
    token_index = (jnp.arange(N_SP, dtype=jnp.int32)[:, None, None] * TOK_DEV + source_entry // TOPK).astype(jnp.int32)
    expert_in = jnp.where(occupied[..., None], normed[token_index], jnp.zeros((), jnp.bfloat16))
    expert_in = jnp.transpose(expert_in, (1, 0, 2, 3)).reshape(EXPERTS, N_SP * CAP, D)
    hidden_group = EFF // N_TP
    slot_rows = N_SP * CAP

    def one_expert(inputs):
        rows, gate_part, up_part, down_part = inputs
        gate_pre = jnp.dot(rows, gate_part, preferred_element_type=jnp.float32)
        up_pre = jnp.dot(rows, up_part, preferred_element_type=jnp.float32)
        hidden = clamped_unit(gate_pre, up_pre)
        hidden_groups = jnp.transpose(hidden.reshape(slot_rows, N_TP, hidden_group), (1, 0, 2))
        down_groups = down_part.reshape(N_TP, hidden_group, D)

        def add_part(running, pieces):
            part_hidden, part_down = pieces
            return (running + round_trip(jnp.dot(part_hidden, part_down, preferred_element_type=jnp.float32)), None)
        summed, _ = lax.scan(add_part, jnp.zeros((slot_rows, D), jnp.float32), (hidden_groups, down_groups))
        return summed.astype(jnp.bfloat16)
    expert_out = lax.map(one_expert, (expert_in, gate_weight, up_weight, down_weight))
    lookup = ((group_routes * N_SP + jnp.arange(N_SP, dtype=jnp.int32)[:, None]) * CAP + slot_index).astype(jnp.int32)
    picked = expert_out.reshape(EXPERTS * slot_rows, D)[lookup.reshape(-1)].reshape(SEQ, TOPK, D).astype(jnp.float32)
    routed = lax.optimization_barrier(jnp.sum(route_weight[:, :, None] * picked, axis=1))
    return (mixed_first + routed).astype(jnp.bfloat16)
```

```python
import functools

import jax
import jax.numpy as jnp
from jax import lax
from jax.experimental import pallas as pl
from jax.experimental.pallas import tpu as pltpu
from jax.sharding import PartitionSpec as P

GRID_W = 64


EPSILON = 1e-06
NEG_BIG = -1e30
ROTARY_BASE = 10000.0
CLAMP_LIMIT = 7.0
SIGMOID_SCALE = 1.702


def rope_tables(positions, head_dim):
    quarter = head_dim // 4
    freqs = ROTARY_BASE ** (-jnp.arange(quarter, dtype=jnp.float32) / quarter)
    row_pos = (positions // GRID_W).astype(jnp.float32)
    col_pos = (positions % GRID_W).astype(jnp.float32)
    angle = jnp.concatenate([row_pos[:, None] * freqs, col_pos[:, None] * freqs], axis=1)
    return (jnp.cos(angle), jnp.sin(angle))


def norm_rotate(heads, gain, cosine_table, sine_table):
    entries = heads.astype(jnp.float32)
    entries = (
        entries * lax.rsqrt(jnp.mean(entries * entries, axis=-1, keepdims=True) + EPSILON) * gain
    )
    pairs = entries.reshape(entries.shape[:-1] + (entries.shape[-1] // 2, 2))
    first = pairs[..., 0]
    second = pairs[..., 1]
    cos_rows = cosine_table[:, None, :]
    sin_rows = sine_table[:, None, :]
    turned = jnp.stack(
        [first * cos_rows - second * sin_rows, first * sin_rows + second * cos_rows], axis=-1
    )
    return turned.reshape(heads.shape).astype(jnp.bfloat16)


def clamped_unit(gate_pre, up_pre):
    bounded = jnp.minimum(gate_pre, CLAMP_LIMIT)
    linear = jnp.clip(up_pre, -CLAMP_LIMIT, CLAMP_LIMIT)
    return (bounded * jax.nn.sigmoid(SIGMOID_SCALE * bounded) * (linear + 1.0)).astype(jnp.bfloat16)


def block_length(length):
    block_size = length
    while block_size > 2048 and block_size % 2 == 0:
        block_size = block_size // 2
    return block_size


def softmax_update(running, inputs, query_rot, own_tags, score_scale):
    row_peak, denominator, carried = running
    key_block, value_block, tag_block = inputs
    scores = (
        jnp.einsum("tkgd,pkd->tkgp", query_rot, key_block, preferred_element_type=jnp.float32)
        * score_scale
    )
    allowed = own_tags[:, None, None, None] == tag_block[None, None, None, :]
    scores = jnp.where(allowed, scores, NEG_BIG)
    new_peak = jnp.maximum(row_peak, jnp.max(scores, axis=-1))
    weights = jnp.where(allowed, jnp.exp(scores - new_peak[..., None]), 0.0)
    factor = jnp.exp(row_peak - new_peak)
    denominator = denominator * factor + jnp.sum(weights, axis=-1)
    carried = carried * factor[..., None] + jnp.einsum(
        "tkgp,pkd->tkgd",
        weights.astype(jnp.bfloat16),
        value_block,
        preferred_element_type=jnp.float32,
    )
    return (new_peak, denominator, carried)


MESH = pl.DeviceIdType.MESH
VMEM_SPEC = pl.BlockSpec(memory_space=pltpu.VMEM)
VMEM_LIMIT = 56 * 1024 * 1024


def remote(src, dst, send_sem, recv_sem, device):
    return pltpu.make_async_remote_copy(
        src_ref=src,
        dst_ref=dst,
        send_sem=send_sem,
        recv_sem=recv_sem,
        device_id=device,
        device_id_type=MESH,
    )


def enter(devices):
    barrier = pltpu.get_barrier_semaphore()
    for device in devices:
        pl.semaphore_signal(barrier, inc=1, device_id=device, device_id_type=MESH)
    pl.semaphore_wait(barrier, len(devices))


def call(kernel, out_shape, scratch, collective, *args):
    return pl.pallas_call(
        kernel,
        out_shape=out_shape,
        in_specs=[VMEM_SPEC] * len(args),
        out_specs=jax.tree.map(lambda _: VMEM_SPEC, out_shape),
        scratch_shapes=scratch,
        compiler_params=pltpu.CompilerParams(
            collective_id=collective, has_side_effects=True, vmem_limit_bytes=VMEM_LIMIT
        ),
    )(*args)


def ring_index(place, n):
    upper = place // (n // 2)
    return (1 - upper) * 2 * place + upper * (2 * (n - 1 - place) + 1)


def gather_kernel(n, pieces, kv_ref, doc_ref, kv_out, doc_out, send, recv, doc_send, doc_recv):
    me, tp = lax.axis_index("sp"), lax.axis_index("tp")
    odd = me % 2
    place = (1 - odd) * (me // 2) + odd * (n - 1 - me // 2)
    right = (ring_index((place + 1) % n, n), tp)
    left = (ring_index((place + n - 1) % n, n), tp)
    enter([((me + d) % n, tp) for d in range(1, n)])
    rows = kv_ref.shape[0] // (2 * pieces)
    copies = []

    def hop(step, chunk):
        forward = chunk < pieces
        origin = (place - step + n) % n if forward else (place + step) % n
        block = ring_index(origin, n)
        span = pl.ds(chunk * rows, rows)
        src = kv_ref.at[span] if step == 0 else kv_out.at[block, span]
        copy = remote(
            src, kv_out.at[block, span], send.at[chunk, step], recv.at[chunk, step],
            right if forward else left,
        )
        copy.start()
        return copy

    order = [c for p in range(pieces) for c in (p, pieces + p)]
    flying = {c: hop(0, c) for c in order}
    doc_copies = []
    for d in range(1, n):
        copy = remote(
            doc_ref, doc_out.at[me], doc_send.at[d], doc_recv.at[d], ((me + d) % n, tp)
        )
        copy.start()
        doc_copies.append(copy)
    kv_out[me] = kv_ref[...]
    doc_out[me] = doc_ref[...]
    for step in range(1, n):
        for c in order:
            flying[c].wait_recv()
            copies.append(flying[c])
            if step < n - 1:
                flying[c] = hop(step, c)
    for copy in copies:
        copy.wait_send()
    for copy in doc_copies:
        copy.wait()


def gather_blocks(kv, docs, n):
    tokens, width = kv.shape
    pieces = 2
    tags = jnp.broadcast_to(docs[None, :], (8, tokens))
    return call(
        functools.partial(gather_kernel, n, pieces),
        (
            jax.ShapeDtypeStruct((n, tokens, width), kv.dtype),
            jax.ShapeDtypeStruct((n, 8, tokens), tags.dtype),
        ),
        [
            pltpu.SemaphoreType.DMA((2 * pieces, n)),
            pltpu.SemaphoreType.DMA((2 * pieces, n)),
            pltpu.SemaphoreType.DMA((n,)),
            pltpu.SemaphoreType.DMA((n,)),
        ],
        0,
        kv,
        tags,
    )


def tp_columns(index, width):
    return pl.ds(pl.multiple_of(index * width, width), width)


def norm_kernel(
    tp_size, part_ref, res_ref, gain_ref, mixed_ref, normed_ref,
    near, outbox, far, sums, sums_in, near_s, near_r, far_s, far_r, sum_s, sum_r,
):
    sp, me = lax.axis_index("sp"), lax.axis_index("tp")
    ys = tp_size // 2
    y, core = me // 2, me % 2
    partner = (sp, y * 2 + 1 - core)
    width = res_ref.shape[1]
    enter([(sp, (me + d) % tp_size) for d in range(1, tp_size)])
    order = list(range(1, ys)) + [0]
    near_copies = {}
    for dy in order:
        cols = tp_columns(((y + dy) % ys) * 2 + 1 - core, width)
        near_copies[dy] = remote(
            part_ref.at[:, cols], near.at[dy], near_s.at[dy], near_r.at[dy], partner
        )
        near_copies[dy].start()
    far_copies = []
    for dy in range(1, ys):
        near_copies[dy].wait_recv()
        own = part_ref[:, tp_columns(((y + dy) % ys) * 2 + core, width)]
        outbox[dy] = (own.astype(jnp.float32) + near[dy].astype(jnp.float32)).astype(jnp.bfloat16)
        copy = remote(
            outbox.at[dy], far.at[dy], far_s.at[dy], far_r.at[dy],
            (sp, ((y + dy) % ys) * 2 + core),
        )
        copy.start()
        far_copies.append(copy)
    near_copies[0].wait_recv()
    total = res_ref[...].astype(jnp.float32) + (
        part_ref[:, tp_columns(me, width)].astype(jnp.float32) + near[0].astype(jnp.float32)
    )
    for dy in range(1, ys):
        far_copies[dy - 1].wait_recv()
        total = total + far[dy].astype(jnp.float32)
    mixed_ref[...] = total
    square = jnp.sum(total * total, axis=1, keepdims=True)
    square = jnp.broadcast_to(square, (square.shape[0], 128)).T
    sums[...] = square[0:8]
    sum_copies = []
    for d in range(1, tp_size):
        copy = remote(
            sums, sums_in.at[d], sum_s.at[d], sum_r.at[d], (sp, (me + d) % tp_size)
        )
        copy.start()
        sum_copies.append(copy)
    full = square[0:8]
    for d in range(1, tp_size):
        sum_copies[d - 1].wait_recv()
        full = full + sums_in[d]
    scale = lax.rsqrt(full / (width * tp_size) + EPSILON)
    scale = jnp.broadcast_to(scale[0:1], (128, full.shape[1])).T[:, 0:1]
    normed_ref[...] = (mixed_ref[...] * scale * gain_ref[...]).astype(jnp.bfloat16)
    for copy in list(near_copies.values()) + far_copies + sum_copies:
        copy.wait_send()


def reduce_and_norm(part, residual, gain, tp_size):
    tokens, width = residual.shape
    ys = tp_size // 2
    block = (ys, tokens, width)
    return call(
        functools.partial(norm_kernel, tp_size),
        (
            jax.ShapeDtypeStruct((tokens, width), jnp.float32),
            jax.ShapeDtypeStruct((tokens, width), jnp.bfloat16),
        ),
        [
            pltpu.VMEM(block, jnp.bfloat16),
            pltpu.VMEM(block, jnp.bfloat16),
            pltpu.VMEM(block, jnp.bfloat16),
            pltpu.VMEM((8, tokens), jnp.float32),
            pltpu.VMEM((tp_size, 8, tokens), jnp.float32),
        ]
        + [pltpu.SemaphoreType.DMA((ys,))] * 4
        + [pltpu.SemaphoreType.DMA((tp_size,))] * 2,
        1,
        part,
        residual,
        gain.reshape(1, width),
    )


def dispatch_kernel(
    n, tp_size, out_ref, rows_ref, hop_s, hop_r, far_s, far_r, near_s, near_r, pass_s, pass_r
):
    me, tp = lax.axis_index("sp"), lax.axis_index("tp")
    ys = tp_size // 2
    y, core = tp // 2, tp % 2
    partner = (me, y * 2 + 1 - core)
    width = out_ref.shape[2]
    mine = tp_columns(tp, width)
    enter(
        [((me + d) % n, tp) for d in range(1, n)]
        + [(me, ((y + dy) % ys) * 2 + core) for dy in range(1, ys)]
        + [partner]
    )

    def hop(d):
        peer = (me + d) % n
        return remote(
            out_ref.at[peer], rows_ref.at[me, :, mine], hop_s.at[d], hop_r.at[d], (peer, tp)
        )

    def far(d, dy):
        block = (me - d + n) % n
        view = rows_ref.at[block, :, mine]
        return remote(
            view, view, far_s.at[d, dy], far_r.at[d, dy], (me, ((y + dy) % ys) * 2 + core)
        )

    def near(d):
        view = rows_ref.at[(me - d + n) % n, :, mine]
        return remote(view, view, near_s.at[d], near_r.at[d], partner)

    def forward(d, dy):
        origin = ((y - dy + ys) % ys) * 2 + core
        view = rows_ref.at[(me - d + n) % n, :, tp_columns(origin, width)]
        return remote(view, view, pass_s.at[d, dy], pass_r.at[d, dy], partner)

    def each(start, stop, body):
        lax.fori_loop(start, stop, lambda i, c: (body(i), c)[1], 0)

    each(1, n, lambda d: hop(d).start())
    rows_ref[me, :, mine] = out_ref[me]

    def spread(d):
        for dy in range(1, ys):
            far(d, dy).start()
        near(d).start()

    def passing(d):
        for dy in range(1, ys):
            far(d, dy).wait_recv()
            forward(d, dy).start()

    spread(0)

    def step(d):
        hop(d).wait_recv()
        spread(d)
        passing(d - 1)

    each(1, n, step)
    passing(n - 1)

    def finish(d):
        near(d).wait()
        for dy in range(1, ys):
            far(d, dy).wait_send()
            forward(d, dy).wait()

    each(0, n, finish)
    each(1, n, lambda d: hop(d).wait_send())


def dispatch_rows(outgoing, n, tp_size):
    _, capacity, width = outgoing.shape
    ys = tp_size // 2
    one, many = (n,), (n, ys)
    sems = [pltpu.SemaphoreType.DMA(shape) for shape in (one, one, many, many) * 2]
    return call(
        functools.partial(dispatch_kernel, n, tp_size),
        jax.ShapeDtypeStruct((n, capacity, width * tp_size), outgoing.dtype),
        sems,
        2,
        outgoing,
    )


def combine_kernel(
    n, tp_size, part_ref, back_ref, near, outbox, far, ready,
    near_s, near_r, far_s, far_r, hop_s, hop_r,
):
    me, tp = lax.axis_index("sp"), lax.axis_index("tp")
    ys = tp_size // 2
    y, core = tp // 2, tp % 2
    partner = (me, y * 2 + 1 - core)
    width = back_ref.shape[2]
    enter(
        [((me + d) % n, tp) for d in range(1, n)]
        + [(me, ((y + dy) % ys) * 2 + core) for dy in range(1, ys)]
        + [partner]
    )

    def near_copy(i, dy):
        block = (me + i + 1) % n
        cols = tp_columns(((y + dy) % ys) * 2 + 1 - core, width)
        return remote(
            part_ref.at[block, :, cols], near.at[i, dy], near_s.at[i, dy], near_r.at[i, dy],
            partner,
        )

    def far_copy(i, dy):
        return remote(
            outbox.at[i, dy], far.at[i, dy], far_s.at[i, dy], far_r.at[i, dy],
            (me, ((y + dy) % ys) * 2 + core),
        )

    def hop_copy(i):
        return remote(
            ready.at[i], back_ref.at[me], hop_s.at[i], hop_r.at[i], ((me + i + 1) % n, tp)
        )

    def each(start, stop, body):
        lax.fori_loop(start, stop, lambda i, c: (body(i), c)[1], 0)

    def begin(i):
        for dy in list(range(1, ys)) + [0]:
            near_copy(i, dy).start()

    def pair_sum(i, dy):
        near_copy(i, dy).wait_recv()
        own = part_ref[(me + i + 1) % n, :, tp_columns(((y + dy) % ys) * 2 + core, width)]
        return own.astype(jnp.float32) + near[i, dy].astype(jnp.float32)

    def across(i):
        for dy in range(1, ys):
            outbox[i, dy] = pair_sum(i, dy).astype(jnp.bfloat16)
            far_copy(i, dy).start()

    def total(i):
        value = pair_sum(i, 0)
        for dy in range(1, ys):
            far_copy(i, dy).wait_recv()
            value = value + far[i, dy].astype(jnp.float32)
        return value.astype(jnp.bfloat16)

    def deliver(i):
        ready[i] = total(i)
        hop_copy(i).start()

    each(0, n, begin)
    lag = min(2, n - 1)
    each(0, lag, across)

    def step(i):
        across(i)
        deliver(i - lag)

    each(lag, n, step)
    each(n - lag, n - 1, deliver)
    back_ref[me] = total(n - 1)

    def finish(i):
        for dy in range(ys):
            near_copy(i, dy).wait_send()
        for dy in range(1, ys):
            far_copy(i, dy).wait_send()

    each(0, n, finish)
    each(0, n - 1, lambda i: hop_copy(i).wait())


def combine_rows(part, n, tp_size):
    _, capacity, full = part.shape
    width = full // tp_size
    ys = tp_size // 2
    many, one = (n, ys), (n,)
    wide = many + (capacity, width)
    return call(
        functools.partial(combine_kernel, n, tp_size),
        jax.ShapeDtypeStruct((n, capacity, width), part.dtype),
        [pltpu.VMEM(wide, jnp.bfloat16)] * 3
        + [pltpu.VMEM((n, capacity, width), jnp.bfloat16)]
        + [pltpu.SemaphoreType.DMA(many)] * 4
        + [pltpu.SemaphoreType.DMA(one)] * 2,
        3,
        part,
    )


def per_device(
    queries,
    keys,
    values,
    docs,
    query_gain,
    key_gain,
    out_weight,
    residual,
    norm_gain,
    routes,
    route_weight,
    gate_weight,
    up_weight,
    down_weight,
):
    tokens = queries.shape[0]
    head_dim = query_gain.shape[0]
    query_heads = queries.shape[1] // head_dim
    pair_heads = keys.shape[1] // head_dim
    pair_width = keys.shape[1]
    positions = lax.axis_index("sp") * tokens + jnp.arange(tokens, dtype=jnp.int32)
    cosine_table, sine_table = rope_tables(positions, head_dim)
    query_rot = norm_rotate(
        queries.reshape(tokens, query_heads, head_dim), query_gain, cosine_table, sine_table
    )
    query_rot = query_rot.reshape(tokens, pair_heads, 2, head_dim)
    key_rot = norm_rotate(
        keys.reshape(tokens, pair_heads, head_dim), key_gain, cosine_table, sine_table
    )
    stacked = jnp.concatenate([key_rot.reshape(tokens, pair_width), values], axis=1)
    own_tags = docs
    score_scale = head_dim ** (-0.5)
    stat_shape = (tokens, pair_heads, 2)
    initial = (
        jnp.full(stat_shape, NEG_BIG, jnp.float32),
        jnp.zeros(stat_shape, jnp.float32),
        jnp.zeros(stat_shape + (head_dim,), jnp.float32),
    )
    groups, ranks = lax.axis_size("sp"), lax.axis_size("tp")
    pair_rows, tag_rows = gather_blocks(stacked, docs, groups)
    pair_rows = pair_rows.reshape(groups * tokens, 2 * pair_width)
    tag_rows = tag_rows[:, 0].reshape(groups * tokens)
    length = pair_rows.shape[0]
    block_size = block_length(length)
    blocks = length // block_size
    key_part = pair_rows[:, :pair_width].reshape(blocks, block_size, pair_heads, head_dim)
    value_part = pair_rows[:, pair_width:].reshape(blocks, block_size, pair_heads, head_dim)
    tag_part = tag_rows.reshape(blocks, block_size)

    def advance(carry_state, inputs):
        return (softmax_update(carry_state, inputs, query_rot, own_tags, score_scale), None)

    result, _ = lax.scan(advance, initial, (key_part, value_part, tag_part))
    row_peak, denominator, carried = result
    attended = (
        (carried / denominator[..., None])
        .astype(jnp.bfloat16)
        .reshape(tokens, query_heads * head_dim)
    )
    width_local = residual.shape[1]
    part = jnp.dot(attended, out_weight, preferred_element_type=jnp.float32).astype(jnp.bfloat16)
    mixed_first, normed = reduce_and_norm(part, residual, norm_gain, ranks)
    experts = lax.axis_size("sp")
    top_count = routes.shape[1]
    capacity = max(2, 5 * tokens * top_count // (4 * experts))
    flat_routes = routes.reshape(-1)
    entries = flat_routes.shape[0]
    expert_ids = jnp.arange(experts, dtype=jnp.int32)
    onehot = (flat_routes[:, None] == expert_ids[None, :]).astype(jnp.int32)
    earlier = jnp.cumsum(onehot, axis=0) - onehot
    slot_index = jnp.sum(earlier * onehot, axis=1)
    slot_ids = jnp.arange(capacity, dtype=jnp.int32)
    matches = (flat_routes[:, None, None] == expert_ids[None, :, None]) & (
        slot_index[:, None, None] == slot_ids[None, None, :]
    )
    entry_ids = jnp.arange(entries, dtype=jnp.int32)
    source_entry = jnp.sum(jnp.where(matches, entry_ids[:, None, None], 0), axis=0)
    occupied = jnp.any(matches, axis=0)
    source_row = source_entry // top_count
    gate_local = gate_weight[0]
    up_local = up_weight[0]
    down_local = down_weight[0]
    model_width = gate_local.shape[0]
    outgoing = jnp.where(occupied[..., None], normed[source_row], jnp.zeros((), jnp.bfloat16))
    arrived = dispatch_rows(outgoing, groups, ranks)
    column_piece = arrived.reshape(-1, model_width)
    gate_pre = jnp.dot(column_piece, gate_local, preferred_element_type=jnp.float32)
    up_pre = jnp.dot(column_piece, up_local, preferred_element_type=jnp.float32)
    hidden = clamped_unit(gate_pre, up_pre)
    partial_value = jnp.dot(hidden, down_local, preferred_element_type=jnp.float32)
    returned = combine_rows(
        partial_value.astype(jnp.bfloat16).reshape(groups, capacity, model_width), groups, ranks
    )
    lookup = flat_routes * capacity + slot_index
    picked = (
        returned.reshape(-1, width_local)[lookup]
        .reshape(tokens, top_count, width_local)
        .astype(jnp.float32)
    )
    routed = jnp.sum(route_weight[:, :, None] * picked, axis=1)
    return (mixed_first + routed).astype(jnp.bfloat16)


def solution(mesh):
    in_specs = (
        P("sp", "tp"),
        P("sp", "tp"),
        P("sp", "tp"),
        P("sp"),
        P(),
        P(),
        P("tp", None),
        P("sp", "tp"),
        P("tp"),
        P("sp", None),
        P("sp", None),
        P("sp", None, "tp"),
        P("sp", None, "tp"),
        P("sp", "tp", None),
    )
    out_specs = P("sp", "tp")
    return jax.shard_map(
        per_device, mesh=mesh, in_specs=in_specs, out_specs=out_specs, check_vma=False
    )
```

```python
import functools

import jax
import jax.numpy as jnp
from jax import lax
from jax.experimental import pallas as pl
from jax.experimental.pallas import tpu as pltpu
from jax.sharding import PartitionSpec as P

GRID_W = 64


EPSILON = 1e-06
NEG_BIG = -1e30
ROTARY_BASE = 10000.0
CLAMP_LIMIT = 7.0
SIGMOID_SCALE = 1.702


def rope_tables(positions, head_dim):
    quarter = head_dim // 4
    freqs = ROTARY_BASE ** (-jnp.arange(quarter, dtype=jnp.float32) / quarter)
    row_pos = (positions // GRID_W).astype(jnp.float32)
    col_pos = (positions % GRID_W).astype(jnp.float32)
    angle = jnp.concatenate([row_pos[:, None] * freqs, col_pos[:, None] * freqs], axis=1)
    return (jnp.cos(angle), jnp.sin(angle))


def norm_rotate(heads, gain, cosine_table, sine_table):
    entries = heads.astype(jnp.float32)
    entries = (
        entries * lax.rsqrt(jnp.mean(entries * entries, axis=-1, keepdims=True) + EPSILON) * gain
    )
    pairs = entries.reshape(entries.shape[:-1] + (entries.shape[-1] // 2, 2))
    first = pairs[..., 0]
    second = pairs[..., 1]
    cos_rows = cosine_table[:, None, :]
    sin_rows = sine_table[:, None, :]
    turned = jnp.stack(
        [first * cos_rows - second * sin_rows, first * sin_rows + second * cos_rows], axis=-1
    )
    return turned.reshape(heads.shape).astype(jnp.bfloat16)


def clamped_unit(gate_pre, up_pre):
    bounded = jnp.minimum(gate_pre, CLAMP_LIMIT)
    linear = jnp.clip(up_pre, -CLAMP_LIMIT, CLAMP_LIMIT)
    return (bounded * jax.nn.sigmoid(SIGMOID_SCALE * bounded) * (linear + 1.0)).astype(jnp.bfloat16)


def block_length(length):
    block_size = length
    while block_size > 2048 and block_size % 2 == 0:
        block_size = block_size // 2
    return block_size


def softmax_update(running, inputs, query_rot, own_tags, score_scale):
    row_peak, denominator, carried = running
    key_block, value_block, tag_block = inputs
    scores = (
        jnp.einsum("tkgd,pkd->tkgp", query_rot, key_block, preferred_element_type=jnp.float32)
        * score_scale
    )
    allowed = own_tags[:, None, None, None] == tag_block[None, None, None, :]
    scores = jnp.where(allowed, scores, NEG_BIG)
    new_peak = jnp.maximum(row_peak, jnp.max(scores, axis=-1))
    weights = jnp.where(allowed, jnp.exp(scores - new_peak[..., None]), 0.0)
    factor = jnp.exp(row_peak - new_peak)
    denominator = denominator * factor + jnp.sum(weights, axis=-1)
    carried = carried * factor[..., None] + jnp.einsum(
        "tkgp,pkd->tkgd",
        weights.astype(jnp.bfloat16),
        value_block,
        preferred_element_type=jnp.float32,
    )
    return (new_peak, denominator, carried)


MESH = pl.DeviceIdType.MESH
VMEM_SPEC = pl.BlockSpec(memory_space=pltpu.VMEM)
VMEM_LIMIT = 56 * 1024 * 1024


def remote(src, dst, send_sem, recv_sem, device):
    return pltpu.make_async_remote_copy(
        src_ref=src,
        dst_ref=dst,
        send_sem=send_sem,
        recv_sem=recv_sem,
        device_id=device,
        device_id_type=MESH,
    )


def enter(devices):
    barrier = pltpu.get_barrier_semaphore()
    for device in devices:
        pl.semaphore_signal(barrier, inc=1, device_id=device, device_id_type=MESH)
    pl.semaphore_wait(barrier, len(devices))


def call(kernel, out_shape, scratch, collective, *args):
    return pl.pallas_call(
        kernel,
        out_shape=out_shape,
        in_specs=[VMEM_SPEC] * len(args),
        out_specs=jax.tree.map(lambda _: VMEM_SPEC, out_shape),
        scratch_shapes=scratch,
        compiler_params=pltpu.CompilerParams(
            collective_id=collective, has_side_effects=True, vmem_limit_bytes=VMEM_LIMIT
        ),
    )(*args)


def ring_index(place, n):
    upper = place // (n // 2)
    return (1 - upper) * 2 * place + upper * (2 * (n - 1 - place) + 1)


def gather_kernel(n, pieces, kv_ref, doc_ref, kv_out, doc_out, send, recv, doc_send, doc_recv):
    me, tp = lax.axis_index("sp"), lax.axis_index("tp")
    odd = me % 2
    place = (1 - odd) * (me // 2) + odd * (n - 1 - me // 2)
    right = (ring_index((place + 1) % n, n), tp)
    left = (ring_index((place + n - 1) % n, n), tp)
    enter([((me + d) % n, tp) for d in range(1, n)])
    rows = kv_ref.shape[0] // (2 * pieces)
    copies = []

    def hop(step, chunk):
        forward = chunk < pieces
        origin = (place - step + n) % n if forward else (place + step) % n
        block = ring_index(origin, n)
        span = pl.ds(chunk * rows, rows)
        src = kv_ref.at[span] if step == 0 else kv_out.at[block, span]
        copy = remote(
            src, kv_out.at[block, span], send.at[chunk, step], recv.at[chunk, step],
            right if forward else left,
        )
        copy.start()
        return copy

    order = [c for p in range(pieces) for c in (p, pieces + p)]
    flying = {c: hop(0, c) for c in order}
    doc_copies = []
    for d in range(1, n):
        copy = remote(
            doc_ref, doc_out.at[me], doc_send.at[d], doc_recv.at[d], ((me + d) % n, tp)
        )
        copy.start()
        doc_copies.append(copy)
    kv_out[me] = kv_ref[...]
    doc_out[me] = doc_ref[...]
    for step in range(1, n):
        for c in order:
            flying[c].wait_recv()
            copies.append(flying[c])
            if step < n - 1:
                flying[c] = hop(step, c)
    for copy in copies:
        copy.wait_send()
    for copy in doc_copies:
        copy.wait()


def gather_blocks(kv, docs, n):
    tokens, width = kv.shape
    pieces = 2
    tags = jnp.broadcast_to(docs[None, :], (8, tokens))
    return call(
        functools.partial(gather_kernel, n, pieces),
        (
            jax.ShapeDtypeStruct((n, tokens, width), kv.dtype),
            jax.ShapeDtypeStruct((n, 8, tokens), tags.dtype),
        ),
        [
            pltpu.SemaphoreType.DMA((2 * pieces, n)),
            pltpu.SemaphoreType.DMA((2 * pieces, n)),
            pltpu.SemaphoreType.DMA((n,)),
            pltpu.SemaphoreType.DMA((n,)),
        ],
        0,
        kv,
        tags,
    )


def tp_columns(index, width):
    return pl.ds(pl.multiple_of(index * width, width), width)


def norm_kernel(
    tp_size, part_ref, res_ref, gain_ref, mixed_ref, normed_ref,
    near, outbox, far, sums, sums_in, near_s, near_r, far_s, far_r, sum_s, sum_r,
):
    sp, me = lax.axis_index("sp"), lax.axis_index("tp")
    ys = tp_size // 2
    y, core = me // 2, me % 2
    partner = (sp, y * 2 + 1 - core)
    width = res_ref.shape[1]
    enter([(sp, (me + d) % tp_size) for d in range(1, tp_size)])
    order = list(range(1, ys)) + [0]
    near_copies = {}
    for dy in order:
        cols = tp_columns(((y + dy) % ys) * 2 + 1 - core, width)
        near_copies[dy] = remote(
            part_ref.at[:, cols], near.at[dy], near_s.at[dy], near_r.at[dy], partner
        )
        near_copies[dy].start()
    far_copies = []
    for dy in range(1, ys):
        near_copies[dy].wait_recv()
        own = part_ref[:, tp_columns(((y + dy) % ys) * 2 + core, width)]
        outbox[dy] = (own.astype(jnp.float32) + near[dy].astype(jnp.float32)).astype(jnp.bfloat16)
        copy = remote(
            outbox.at[dy], far.at[dy], far_s.at[dy], far_r.at[dy],
            (sp, ((y + dy) % ys) * 2 + core),
        )
        copy.start()
        far_copies.append(copy)
    near_copies[0].wait_recv()
    total = res_ref[...].astype(jnp.float32) + (
        part_ref[:, tp_columns(me, width)].astype(jnp.float32) + near[0].astype(jnp.float32)
    )
    for dy in range(1, ys):
        far_copies[dy - 1].wait_recv()
        total = total + far[dy].astype(jnp.float32)
    mixed_ref[...] = total
    square = jnp.sum(total * total, axis=1, keepdims=True)
    square = jnp.broadcast_to(square, (square.shape[0], 128)).T
    sums[...] = square[0:8]
    sum_copies = []
    for d in range(1, tp_size):
        copy = remote(
            sums, sums_in.at[d], sum_s.at[d], sum_r.at[d], (sp, (me + d) % tp_size)
        )
        copy.start()
        sum_copies.append(copy)
    full = square[0:8]
    for d in range(1, tp_size):
        sum_copies[d - 1].wait_recv()
        full = full + sums_in[d]
    scale = lax.rsqrt(full / (width * tp_size) + EPSILON)
    scale = jnp.broadcast_to(scale[0:1], (128, full.shape[1])).T[:, 0:1]
    normed_ref[...] = (mixed_ref[...] * scale * gain_ref[...]).astype(jnp.bfloat16)
    for copy in list(near_copies.values()) + far_copies + sum_copies:
        copy.wait_send()


def reduce_and_norm(part, residual, gain, tp_size):
    tokens, width = residual.shape
    ys = tp_size // 2
    block = (ys, tokens, width)
    return call(
        functools.partial(norm_kernel, tp_size),
        (
            jax.ShapeDtypeStruct((tokens, width), jnp.float32),
            jax.ShapeDtypeStruct((tokens, width), jnp.bfloat16),
        ),
        [
            pltpu.VMEM(block, jnp.bfloat16),
            pltpu.VMEM(block, jnp.bfloat16),
            pltpu.VMEM(block, jnp.bfloat16),
            pltpu.VMEM((8, tokens), jnp.float32),
            pltpu.VMEM((tp_size, 8, tokens), jnp.float32),
        ]
        + [pltpu.SemaphoreType.DMA((ys,))] * 4
        + [pltpu.SemaphoreType.DMA((tp_size,))] * 2,
        1,
        part,
        residual,
        gain.reshape(1, width),
    )


def expert_kernel(
    n, tp_size, out_ref, gate_hbm, up_hbm, down_hbm, back_ref,
    rows, gate, up, down, hidden, part, near, outbox, far, ready, load_sem,
    in_s, in_r, side_s, side_r, back_s, back_r,
    cross_s, cross_r, pass_s, pass_r, near_s, near_r, far_s, far_r,
):
    me, tp = lax.axis_index("sp"), lax.axis_index("tp")
    ys = tp_size // 2
    y, core = tp // 2, tp % 2
    partner = (me, y * 2 + 1 - core)
    width = out_ref.shape[2]
    mine = tp_columns(tp, width)
    loads = [
        pltpu.make_async_copy(src.at[0], dst, load_sem.at[i])
        for i, (src, dst) in enumerate(((gate_hbm, gate), (up_hbm, up), (down_hbm, down)))
    ]
    for load in loads:
        load.start()
    enter(
        [((me + d) % n, tp) for d in range(1, n)]
        + [(me, ((y + dy) % ys) * 2 + core) for dy in range(1, ys)]
        + [partner]
    )

    def source(d):
        return (me - d + n) % n

    def across_y(dy):
        return (me, ((y + dy) % ys) * 2 + core)

    def hop_in(d):
        peer = (me + d) % n
        return remote(
            out_ref.at[peer], rows.at[me, :, mine], in_s.at[d], in_r.at[d], (peer, tp)
        )

    def cross(d, dy):
        view = rows.at[source(d), :, mine]
        return remote(view, view, cross_s.at[d, dy], cross_r.at[d, dy], across_y(dy))

    def side(d):
        view = rows.at[source(d), :, mine]
        return remote(view, view, side_s.at[d], side_r.at[d], partner)

    def forward(d, dy):
        origin = ((y - dy + ys) % ys) * 2 + core
        view = rows.at[source(d), :, tp_columns(origin, width)]
        return remote(view, view, pass_s.at[d, dy], pass_r.at[d, dy], partner)

    def near_copy(d, dy):
        cols = tp_columns(((y + dy) % ys) * 2 + 1 - core, width)
        return remote(
            part.at[d, :, cols], near.at[d, dy], near_s.at[d, dy], near_r.at[d, dy], partner
        )

    def far_copy(d, dy):
        return remote(
            outbox.at[d, dy], far.at[d, dy], far_s.at[d, dy], far_r.at[d, dy], across_y(dy)
        )

    def hop_back(d):
        return remote(
            ready.at[d], back_ref.at[me], back_s.at[d], back_r.at[d], (source(d), tp)
        )

    def each(start, stop, body):
        lax.fori_loop(start, stop, lambda i, c: (body(i), c)[1], 0)

    def spread(d):
        @pl.when(d > 0)
        def _():
            hop_in(d).wait_recv()

        for dy in range(1, ys):
            cross(d, dy).start()
        side(d).start()

    def relay(d):
        for dy in range(1, ys):
            cross(d, dy).wait_recv()
            forward(d, dy).start()

    def compute(d):
        @pl.when(d == 0)
        def _():
            for load in loads:
                load.wait()

        side(d).wait_recv()
        for dy in range(1, ys):
            forward(d, dy).wait_recv()
        block = rows[source(d)]
        units = gate.shape[1]
        piece = min(256, units)
        for start in range(0, units, piece):
            span = slice(start, start + piece)
            gate_pre = jnp.dot(block, gate[:, span], preferred_element_type=jnp.float32)
            up_pre = jnp.dot(block, up[:, span], preferred_element_type=jnp.float32)
            hidden[:, span] = clamped_unit(gate_pre, up_pre)
        units_in = hidden[...]
        for t in range(tp_size):
            span = slice(t * width, (t + 1) * width)
            part[d, :, span] = jnp.dot(
                units_in, down[:, span], preferred_element_type=jnp.float32
            ).astype(jnp.bfloat16)
        for dy in list(range(1, ys)) + [0]:
            near_copy(d, dy).start()

    def pair_sum(d, dy):
        near_copy(d, dy).wait_recv()
        own = part[d, :, tp_columns(((y + dy) % ys) * 2 + core, width)]
        return own.astype(jnp.float32) + near[d, dy].astype(jnp.float32)

    def reduce_pair(d):
        for dy in range(1, ys):
            outbox[d, dy] = pair_sum(d, dy).astype(jnp.bfloat16)
            far_copy(d, dy).start()

    def deliver(d):
        value = pair_sum(d, 0)
        for dy in range(1, ys):
            far_copy(d, dy).wait_recv()
            value = value + far[d, dy].astype(jnp.float32)
        ready[d] = value.astype(jnp.bfloat16)

        @pl.when(d > 0)
        def _():
            hop_back(d).start()

    stages = ((spread, 0), (relay, 1), (reduce_pair, 3), (deliver, 4), (compute, 2))

    def step(k):
        for stage, lag in stages:
            @pl.when((k >= lag) & (k < n + lag))
            def _(stage=stage, lag=lag):
                stage(k - lag)

    each(1, n, lambda d: hop_in(d).start())
    rows[me, :, mine] = out_ref[me]
    each(0, n + 4, step)
    back_ref[me] = ready[0]

    def finish(d):
        side(d).wait_send()
        for dy in range(1, ys):
            cross(d, dy).wait_send()
            forward(d, dy).wait_send()
            far_copy(d, dy).wait_send()
        for dy in range(ys):
            near_copy(d, dy).wait_send()

    def finish_hops(d):
        hop_in(d).wait_send()
        hop_back(d).wait()

    each(0, n, finish)
    each(1, n, finish_hops)


def run_experts(outgoing, gate_weight, up_weight, down_weight, n, tp_size):
    _, capacity, width = outgoing.shape
    ys = tp_size // 2
    full, units = gate_weight.shape[1:]
    wide = (n, ys, capacity, width)
    kind = outgoing.dtype
    shapes = [
        (n, capacity, full),
        (full, units),
        (full, units),
        (units, full),
        (capacity, units),
        (n, capacity, full),
        wide,
        wide,
        wide,
        (n, capacity, width),
    ]
    sems = [(3,)] + [(n,)] * 6 + [(n, ys)] * 8
    return pl.pallas_call(
        functools.partial(expert_kernel, n, tp_size),
        out_shape=jax.ShapeDtypeStruct((n, capacity, width), kind),
        in_specs=[VMEM_SPEC] + [pl.BlockSpec(memory_space=pl.ANY)] * 3,
        out_specs=VMEM_SPEC,
        scratch_shapes=[pltpu.VMEM(shape, kind) for shape in shapes]
        + [pltpu.SemaphoreType.DMA(shape) for shape in sems],
        compiler_params=pltpu.CompilerParams(
            collective_id=2, has_side_effects=True, vmem_limit_bytes=VMEM_LIMIT
        ),
    )(outgoing, gate_weight, up_weight, down_weight)


def per_device(
    queries,
    keys,
    values,
    docs,
    query_gain,
    key_gain,
    out_weight,
    residual,
    norm_gain,
    routes,
    route_weight,
    gate_weight,
    up_weight,
    down_weight,
):
    tokens = queries.shape[0]
    head_dim = query_gain.shape[0]
    query_heads = queries.shape[1] // head_dim
    pair_heads = keys.shape[1] // head_dim
    pair_width = keys.shape[1]
    positions = lax.axis_index("sp") * tokens + jnp.arange(tokens, dtype=jnp.int32)
    cosine_table, sine_table = rope_tables(positions, head_dim)
    query_rot = norm_rotate(
        queries.reshape(tokens, query_heads, head_dim), query_gain, cosine_table, sine_table
    )
    query_rot = query_rot.reshape(tokens, pair_heads, 2, head_dim)
    key_rot = norm_rotate(
        keys.reshape(tokens, pair_heads, head_dim), key_gain, cosine_table, sine_table
    )
    stacked = jnp.concatenate([key_rot.reshape(tokens, pair_width), values], axis=1)
    own_tags = docs
    score_scale = head_dim ** (-0.5)
    stat_shape = (tokens, pair_heads, 2)
    initial = (
        jnp.full(stat_shape, NEG_BIG, jnp.float32),
        jnp.zeros(stat_shape, jnp.float32),
        jnp.zeros(stat_shape + (head_dim,), jnp.float32),
    )
    groups, ranks = lax.axis_size("sp"), lax.axis_size("tp")
    pair_rows, tag_rows = gather_blocks(stacked, docs, groups)
    pair_rows = pair_rows.reshape(groups * tokens, 2 * pair_width)
    tag_rows = tag_rows[:, 0].reshape(groups * tokens)
    length = pair_rows.shape[0]
    block_size = block_length(length)
    blocks = length // block_size
    key_part = pair_rows[:, :pair_width].reshape(blocks, block_size, pair_heads, head_dim)
    value_part = pair_rows[:, pair_width:].reshape(blocks, block_size, pair_heads, head_dim)
    tag_part = tag_rows.reshape(blocks, block_size)

    def advance(carry_state, inputs):
        return (softmax_update(carry_state, inputs, query_rot, own_tags, score_scale), None)

    result, _ = lax.scan(advance, initial, (key_part, value_part, tag_part))
    row_peak, denominator, carried = result
    attended = (
        (carried / denominator[..., None])
        .astype(jnp.bfloat16)
        .reshape(tokens, query_heads * head_dim)
    )
    width_local = residual.shape[1]
    part = jnp.dot(attended, out_weight, preferred_element_type=jnp.float32).astype(jnp.bfloat16)
    mixed_first, normed = reduce_and_norm(part, residual, norm_gain, ranks)
    experts = lax.axis_size("sp")
    top_count = routes.shape[1]
    capacity = max(2, 5 * tokens * top_count // (4 * experts))
    flat_routes = routes.reshape(-1)
    entries = flat_routes.shape[0]
    expert_ids = jnp.arange(experts, dtype=jnp.int32)
    onehot = (flat_routes[:, None] == expert_ids[None, :]).astype(jnp.int32)
    earlier = jnp.cumsum(onehot, axis=0) - onehot
    slot_index = jnp.sum(earlier * onehot, axis=1)
    lookup = (flat_routes * capacity + slot_index).reshape(tokens, top_count)
    slot_ids = jnp.arange(experts * capacity, dtype=jnp.int32)
    holds = lookup[:, :, None] == slot_ids[None, None, :]
    chosen = jnp.any(holds, axis=1).astype(jnp.bfloat16)
    mixing = jnp.sum(jnp.where(holds, route_weight[:, :, None], 0.0), axis=1)
    mixing_high = lax.reduce_precision(mixing, 8, 7)
    mixing_low = (mixing - mixing_high).astype(jnp.bfloat16)
    mixing_high = mixing_high.astype(jnp.bfloat16)
    outgoing = lax.dot_general(
        chosen, normed, (((0,), (0,)), ((), ())), preferred_element_type=jnp.float32
    ).astype(jnp.bfloat16).reshape(experts, capacity, width_local)
    returned = run_experts(outgoing, gate_weight, up_weight, down_weight, groups, ranks)
    returned = returned.reshape(experts * capacity, width_local)
    routed = jnp.dot(mixing_high, returned, preferred_element_type=jnp.float32) + jnp.dot(
        mixing_low, returned, preferred_element_type=jnp.float32
    )
    return (mixed_first + routed).astype(jnp.bfloat16)


def solution(mesh):
    in_specs = (
        P("sp", "tp"),
        P("sp", "tp"),
        P("sp", "tp"),
        P("sp"),
        P(),
        P(),
        P("tp", None),
        P("sp", "tp"),
        P("tp"),
        P("sp", None),
        P("sp", None),
        P("sp", None, "tp"),
        P("sp", None, "tp"),
        P("sp", "tp", None),
    )
    out_specs = P("sp", "tp")
    return jax.shard_map(
        per_device, mesh=mesh, in_specs=in_specs, out_specs=out_specs, check_vma=False
    )
```
